32 devices in a mesh: kv: 8 (over z, x), tp: 4 (over y, core).
Axes of the slice: x: 2, y: 2, z: 4, core: 2. Of those that a mesh axis runs over, the one named last changes fastest.
Arguments:
- tokens: bfloat16 [22, 4096], P(None, ('kv', 'tp')), may hold values from -22 to 22
- attn_gain: float32 [4096], P('kv'), may hold values from 0.1 to 1.9
- w_query: bfloat16 [4096, 4096], P('kv', 'tp'), may hold values from -0.09375 to 0.09375
- w_key: bfloat16 [4096, 4096], P('kv', 'tp'), may hold values from -0.5 to 0.5
- w_value: bfloat16 [4096, 4096], P('kv', 'tp'), may hold values from -0.09375 to 0.09375
- cache_keys: bfloat16 [22, 2048, 32, 128], P(None, 'kv', 'tp'), may hold values from -256 to 256
- cache_values: bfloat16 [22, 2048, 32, 128], P(None, 'kv', 'tp'), may hold values from -6 to 6
- lambdas: float32 [32], P('tp'), may hold values from 0.3 to 0.8
- head_gain: float32 [128], replicated, may hold values from 0.1 to 1.9
- w_out: bfloat16 [4096, 4096], P('tp', 'kv'), may hold values from -0.09375 to 0.09375
- mlp_gain: float32 [4096], P('kv'), may hold values from 0.1 to 1.9
- w_gate: bfloat16 [4096, 11008], P('kv', 'tp'), may hold values from -0.09375 to 0.09375
- w_up: bfloat16 [4096, 11008], P('kv', 'tp'), may hold values from -0.09375 to 0.09375
- w_down: bfloat16 [11008, 4096], P('tp', 'kv'), may hold values from -0.0546875 to 0.0546875
Outputs:
- output: bfloat16 [22, 4096], P(None, ('kv', 'tp'))
The draws below stay inside these ranges and needn't reach their ends.
All inputs are finite; a program needn't handle non-finite values.
Results may differ from the reference program's by a relative error of at most 0.017.
The reference program's roundings to bfloat16 on the way (of `normed_in`, `query_all`, `heads_out`, `residual`, `normed_mid` and `hidden`) count: a program that leaves them out, or rounds other values in their place, can miss the bound.
Values may be sent and summed in bfloat16 or wider, within the bound.
A program may use at most 128 MiB of HBM per device.

```python
import jax
import jax.numpy as jnp
from jax import lax

D = 4096
HEADS = 32
HEAD_DIM = 128
HALF = 64
FF = 11008
SEQS = 22
POS_DEV = 256
CACHE_LEN = 2048
N_KV = 8
N_TP = 4


def draw_tokens(key, part):
    key_base = jax.random.fold_in(key, 11)
    key_rows = jax.random.fold_in(key, 12)
    columns = jnp.arange(D, dtype=jnp.float32) / (D - 1)
    base_vals = jnp.clip(jax.random.normal(key_base, (SEQS, D), jnp.float32), -4.0, 4.0)
    col_scale = jnp.exp(jnp.log(3.0) * (columns - 0.5))
    row_scale = jnp.exp(jax.random.uniform(key_rows, (SEQS, 1), jnp.float32, jnp.log(1.0 / 3.0), jnp.log(3.0)))
    return (base_vals * row_scale * col_scale[None, :]).astype(jnp.bfloat16)


def draw_cache_keys(key, part):
    key_base = jax.random.fold_in(key, 21)
    base_vals = jnp.clip(jax.random.normal(key_base, (SEQS, CACHE_LEN, HEADS, HEAD_DIM), jnp.float32), -6.0, 6.0) * 1.75
    return base_vals.astype(jnp.bfloat16)


def block_levels(rng, shape, cuts, low, high):
    loudness, own = 1.0, jax.random.fold_in(rng, 6)
    for axis_at, blocks in cuts:
        steps = jnp.exp(jax.random.uniform(jax.random.fold_in(own, axis_at), (blocks,), jnp.float32, low / len(cuts), high / len(cuts)))
        loudness = loudness * jnp.repeat(steps, shape[axis_at] // blocks).reshape([-1 if axis == axis_at else 1 for axis in range(len(shape))])
    return loudness


def bell_draw(key, dims, spread, bound, split=(), kind=jnp.bfloat16):
    level = block_levels(key, dims, split, -0.22, 0.18) if split else 1.0
    entries = jax.random.normal(key, dims, jnp.float32) * spread * level
    return jnp.minimum(jnp.maximum(entries, -bound), bound).astype(kind)


def setup_inputs(seed: int = 0) -> dict:
    key_of = jax.random.split(jax.random.key(seed), 15)
    tokens = draw_tokens(jax.random.fold_in(key_of[14], 71), 0)
    attn_gain = jnp.clip(1.0 + 0.18 * jax.random.normal(key_of[1], (D,), jnp.float32), 0.1, 1.9)
    w_query = bell_draw(key_of[2], (D, HEADS * HEAD_DIM), D ** -0.5, 0.09375, ((0, 8), (1, 4)))
    w_key = bell_draw(key_of[3], (D, HEADS * HEAD_DIM), (D // 36) ** -0.5, 0.5, ((0, 8), (1, 4)))
    w_value = bell_draw(key_of[4], (D, HEADS * HEAD_DIM), D ** -0.5, 0.09375, ((0, 8), (1, 4)))
    cache_keys = draw_cache_keys(jax.random.fold_in(key_of[14], 71), 0)
    cache_values = bell_draw(key_of[6], (SEQS, CACHE_LEN, HEADS, HEAD_DIM), 1.0, 6.0, ((1, 8), (2, 4)))
    lambdas = jnp.clip(0.3 + 0.5 * jax.random.uniform(key_of[7], (HEADS,), jnp.float32) ** block_levels(key_of[7], (HEADS,), ((0, 4),), -0.2, 0.2), 0.3, 0.8)
    head_gain = jnp.clip(1.0 + 0.18 * jax.random.normal(key_of[8], (HEAD_DIM,), jnp.float32), 0.1, 1.9)
    w_out = bell_draw(key_of[9], (HEADS * HEAD_DIM, D), (HEADS * HEAD_DIM) ** -0.5, 0.09375, ((0, 4), (1, 8)))
    mlp_gain = jnp.clip(1.0 + 0.18 * jax.random.normal(key_of[10], (D,), jnp.float32), 0.1, 1.9)
    w_gate = bell_draw(key_of[11], (D, FF), D ** -0.5, 0.09375, ((0, 8), (1, 4)))
    w_up = bell_draw(key_of[12], (D, FF), D ** -0.5, 0.09375, ((0, 8), (1, 4)))
    w_down = bell_draw(key_of[13], (FF, D), FF ** -0.5, 0.0546875, ((0, 4), (1, 8)))
    return dict(tokens=tokens, attn_gain=attn_gain, w_query=w_query, w_key=w_key, w_value=w_value, cache_keys=cache_keys, cache_values=cache_values, lambdas=lambdas, head_gain=head_gain, w_out=w_out, mlp_gain=mlp_gain, w_gate=w_gate, w_up=w_up, w_down=w_down)


epsilon = 1e-06

def blocked_attention(query_vec, key_new, value_new, keys_head, values_head, low, high):
    seq_count = keys_head.shape[0]
    score_scale = HALF ** (-0.5)
    query_part = query_vec[:, low:high].astype(jnp.float32)
    scores = jnp.einsum('sd,std->st', query_part, keys_head[:, :, low:high].astype(jnp.float32)) * score_scale
    score_new = lax.optimization_barrier(jnp.sum(query_part * key_new[:, low:high].astype(jnp.float32), axis=1)) * score_scale
    blocks = scores.reshape(seq_count, N_KV, POS_DEV)
    maxima = lax.optimization_barrier(jnp.max(blocks, axis=2))
    weights = jnp.exp(blocks - maxima[:, :, None])
    totals = lax.optimization_barrier(jnp.sum(weights, axis=2))
    rounded = lax.optimization_barrier(weights.astype(jnp.bfloat16)).astype(jnp.float32)
    blocked_values = values_head.astype(jnp.float32).reshape(seq_count, N_KV, POS_DEV, HEAD_DIM)
    sums = jnp.einsum('snt,sntd->snd', rounded, blocked_values)
    peak = jnp.maximum(lax.optimization_barrier(jnp.max(maxima, axis=1)), score_new)
    block_weight = jnp.exp(maxima - peak[:, None])
    new_weight = jnp.exp(score_new - peak)
    denominator = lax.optimization_barrier(jnp.sum(block_weight * totals, axis=1)) + new_weight
    numerator = lax.optimization_barrier(jnp.sum(block_weight[:, :, None] * sums, axis=1)) + new_weight[:, None] * value_new.astype(jnp.float32)
    return numerator / denominator[:, None]

def grouped_product(activations, weights_mat, groups):
    span_rows = weights_mat.shape[0] // groups
    result = jnp.zeros((activations.shape[0], weights_mat.shape[1]), jnp.float32)
    for block_index in range(groups):
        partial_value = jnp.dot(activations[:, block_index * span_rows:(block_index + 1) * span_rows], weights_mat[block_index * span_rows:(block_index + 1) * span_rows], preferred_element_type=jnp.float32)
        result = result + lax.optimization_barrier(partial_value.astype(jnp.bfloat16)).astype(jnp.float32)
    return result

def reference(tokens, attn_gain, w_query, w_key, w_value, cache_keys, cache_values, lambdas, head_gain, w_out, mlp_gain, w_gate, w_up, w_down):
    seq_count = tokens.shape[0]
    tokens_f = tokens.astype(jnp.float32)
    scale_in = lax.rsqrt(lax.optimization_barrier(jnp.mean(tokens_f * tokens_f, axis=1, keepdims=True)) + epsilon)
    normed_in = (tokens_f * attn_gain.astype(jnp.float32)).astype(jnp.bfloat16)

    def project(weight):
        product = jnp.dot(normed_in, weight, preferred_element_type=jnp.float32)
        return (scale_in * product).astype(jnp.bfloat16).reshape(seq_count, HEADS, HEAD_DIM)
    query_all = project(w_query)
    key_all = project(w_key)
    value_all = project(w_value)

    def one_head(head_index):
        keys_head = lax.dynamic_index_in_dim(cache_keys, head_index, 2, keepdims=False)
        values_head = lax.dynamic_index_in_dim(cache_values, head_index, 2, keepdims=False)
        query_vec = lax.dynamic_index_in_dim(query_all, head_index, 1, keepdims=False)
        key_new = lax.dynamic_index_in_dim(key_all, head_index, 1, keepdims=False)
        value_new = lax.dynamic_index_in_dim(value_all, head_index, 1, keepdims=False)
        first_map = blocked_attention(query_vec, key_new, value_new, keys_head, values_head, 0, HALF)
        second_map = blocked_attention(query_vec, key_new, value_new, keys_head, values_head, HALF, HEAD_DIM)
        return (first_map, second_map)
    first_map, second_map = lax.map(one_head, jnp.arange(HEADS, dtype=jnp.int32))
    difference = first_map - lambdas.astype(jnp.float32)[:, None, None] * second_map
    normed = difference * lax.rsqrt(lax.optimization_barrier(jnp.mean(difference * difference, axis=2, keepdims=True)) + epsilon)
    normed = normed * head_gain.astype(jnp.float32)
    heads_out = jnp.transpose(normed, (1, 0, 2)).reshape(seq_count, HEADS * HEAD_DIM).astype(jnp.bfloat16)
    branch = grouped_product(heads_out, w_out, N_TP)
    residual = (tokens_f + branch).astype(jnp.bfloat16)
    residual_f = residual.astype(jnp.float32)
    scale_mid = lax.rsqrt(lax.optimization_barrier(jnp.mean(residual_f * residual_f, axis=1, keepdims=True)) + epsilon)
    normed_mid = (residual_f * mlp_gain.astype(jnp.float32)).astype(jnp.bfloat16)
    gate = scale_mid * jnp.dot(normed_mid, w_gate, preferred_element_type=jnp.float32)
    up_val = scale_mid * jnp.dot(normed_mid, w_up, preferred_element_type=jnp.float32)
    hidden = (jax.nn.silu(gate) * up_val).astype(jnp.bfloat16)
    mixer = grouped_product(hidden, w_down, N_TP)
    return (residual_f + mixer).astype(jnp.bfloat16)
```

```python
import functools

import jax
import jax.numpy as jnp
from jax import lax
from jax.experimental import pallas as pl
from jax.experimental.pallas import tpu as pltpu
from jax.sharding import PartitionSpec as P

epsilon = 1e-06
MESH = pl.DeviceIdType.MESH
F32 = jnp.float32
BF16 = jnp.bfloat16
QKV_LINK = jnp.float32
FF_LINK = jnp.bfloat16


def peers(axis, count):
    me = lax.axis_index(axis)
    return [(step, lax.rem(me + step, count)) for step in range(1, count)]


def greet(n_kv, n_tp):
    barrier = pltpu.get_barrier_semaphore()
    for axis, count in (("kv", n_kv), ("tp", n_tp)):
        for _, peer in peers(axis, count):
            pl.semaphore_signal(barrier, inc=1, device_id={axis: peer}, device_id_type=MESH)
    pl.semaphore_wait(barrier, n_kv + n_tp - 2)


def exchange(axis, count, source, target, send_sem, recv_sem):
    copies = []
    for step, peer in peers(axis, count):
        copy = pltpu.make_async_remote_copy(
            src_ref=source(peer),
            dst_ref=target,
            send_sem=send_sem.at[step - 1],
            recv_sem=recv_sem.at[step - 1],
            device_id={axis: peer},
            device_id_type=MESH,
        )
        copy.start()
        copies.append(copy)
    return copies


def wait_recv(copies):
    for copy in copies:
        copy.wait_recv()


def wait_send(copies):
    for copy in copies:
        copy.wait_send()


def pad_rows(value, rows):
    if value.shape[0] == rows:
        return value
    return jnp.concatenate(
        [value, jnp.zeros((rows - value.shape[0],) + value.shape[1:], value.dtype)], axis=0
    )


def pad_cols(value, cols):
    if value.shape[1] == cols:
        return value
    return jnp.concatenate(
        [value, jnp.zeros((value.shape[0], cols - value.shape[1]), value.dtype)], axis=1
    )


def project_kernel(
    dims, tok, gain, wq, wk, wv, x_out, q_out, k_out, v_out,
    wbuf, tok_all, sq_all, part, got, w_sem, t_s, t_r, s_s, s_r, p_s, p_r, q_s, q_r,
):
    n_kv, n_tp, groups, rows, width = dims
    seqs = tok.shape[0]
    hd = q_out.shape[2]
    loads = []
    for index, ref in enumerate((wq, wk, wv)):
        load = pltpu.make_async_copy(ref, wbuf.at[index], w_sem.at[index])
        load.start()
        loads.append(load)
    greet(n_kv, n_tp)
    me = lax.axis_index("kv")
    me_tp = lax.axis_index("tp")
    tok_copies = exchange("tp", n_tp, lambda peer: tok, tok_all.at[me_tp], t_s, t_r)
    tok_all[me_tp] = tok[...]
    wait_recv(tok_copies)
    x = jnp.concatenate([tok_all[index] for index in range(n_tp)], axis=1)
    x_out[...] = x
    xf = x.astype(F32)
    sq_all[me] = jnp.broadcast_to(jnp.sum(xf * xf, axis=1, keepdims=True), (seqs, 128))
    sq_copies = exchange("kv", n_kv, lambda peer: sq_all.at[me], sq_all.at[me], s_s, s_r)
    normed = (xf * gain[...]).astype(BF16)
    for index in range(3):
        loads[index].wait()
        product = jnp.dot(normed, wbuf[index], preferred_element_type=F32).astype(QKV_LINK)
        product = pad_rows(product, groups * rows)
        for owner in range(n_kv):
            head, group = owner // groups, owner % groups
            part[owner, index] = product[
                group * rows : (group + 1) * rows, head * hd : (head + 1) * hd
            ]
    part_copies = exchange("kv", n_kv, lambda peer: part.at[peer], got.at[me], p_s, p_r)
    got[me] = part[me]
    wait_recv(sq_copies)
    square = sq_all[0]
    for index in range(1, n_kv):
        square = square + sq_all[index]
    scale = lax.rsqrt(square[:, :1] / width + epsilon)
    if groups > 1:
        scale = pad_rows(scale, groups * rows)
        group_of = lax.rem(me, groups)
        mine = scale[:rows]
        for group in range(1, groups):
            mine = jnp.where(group_of == group, scale[group * rows : (group + 1) * rows], mine)
        scale = mine
    wait_recv(part_copies)
    for index in range(3):
        total = got[0, index].astype(F32)
        for owner in range(1, n_kv):
            total = total + got[owner, index].astype(F32)
        value = (scale * total).astype(BF16)
        if index == 0:
            q_out[me] = value
            q_copies = exchange("kv", n_kv, lambda peer: q_out.at[me], q_out.at[me], q_s, q_r)
        elif index == 1:
            k_out[...] = value
        else:
            v_out[...] = value
    wait_recv(q_copies)
    wait_send(tok_copies + sq_copies + part_copies + q_copies)


def attend_kernel(heads, per_step, q, keys, values, o_out, l_out, acc, lse):
    step = pl.program_id(0)
    length = keys.shape[1]
    hd = keys.shape[2]
    scale = (hd // 2) ** (-0.5)
    row = lax.broadcasted_iota(jnp.int32, (2 * heads, length), 0)
    col = lax.broadcasted_iota(jnp.int32, (2 * heads, length), 1)
    keep = lax.rem(col, heads) == lax.rem(row, heads)
    lane = lax.broadcasted_iota(jnp.int32, (2 * heads, 128), 1)

    @pl.when(step == 0)
    def _():
        lse[...] = jnp.zeros_like(lse)

    for index in range(per_step):
        seq = step * per_step + index
        scores = lax.dot_general(
            q[index], keys[index], (((1,), (1,)), ((), ())), preferred_element_type=F32
        )
        scores = jnp.where(keep, scores * scale, -1e30)
        peak = jnp.max(scores, axis=1, keepdims=True)
        weights = jnp.where(keep, jnp.exp(scores - peak), 0.0)
        total = jnp.sum(weights, axis=1, keepdims=True)
        summed = jnp.dot(weights.astype(BF16), values[index], preferred_element_type=F32)
        result = summed / total
        acc[:, pl.ds(seq, 1), :] = result[:, None, :]
        lse[...] = jnp.where(lane == seq, peak + jnp.log(total), lse[...])

    @pl.when(step == pl.num_programs(0) - 1)
    def _():
        stats = lse[...]
        l_out[...] = jnp.zeros_like(l_out)
        for head in range(heads):
            for half in range(2):
                at = half * heads + head
                o_out[head, half] = acc[at].astype(BF16)
                l_out[head, half : half + 1, :] = stats[at : at + 1, :]


def finish_kernel(
    dims, lam, o_in, l_in, q_all, k_own, v_own, head_gain, x, mid_gain, w_out, w_gate, w_up, w_down,
    out,
    wo, wg, wu, wd, o_all, l_all, h_all, b_all, sq_all, gu_part, gu_all, hid_all, d_part, d_all,
    w_sem, o_s, o_r, l_s, l_r, h_s, h_r, b_s, b_r, s_s, s_r, g_s, g_r, i_s, i_r, d_s, d_r,
):
    n_kv, n_tp, groups, rows, width, chunk = dims
    seqs = x.shape[0]
    hd = k_own.shape[1]
    loads = []
    for index, (ref, buf) in enumerate(((w_out, wo), (w_gate, wg), (w_up, wu), (w_down, wd))):
        load = pltpu.make_async_copy(ref, buf, w_sem.at[index])
        load.start()
        loads.append(load)
    greet(n_kv, n_tp)
    me = lax.axis_index("kv")
    me_tp = lax.axis_index("tp")
    l_copies = exchange("kv", n_kv, lambda peer: l_in.at[peer], l_all.at[me], l_s, l_r)
    o_copies = exchange("kv", n_kv, lambda peer: o_in.at[peer], o_all.at[me], o_s, o_r)
    l_all[me] = l_in[me]
    o_all[me] = o_in[me]
    product = q_all[me].astype(F32) * k_own[...].astype(F32)
    lane = lax.broadcasted_iota(jnp.int32, product.shape, 1)
    low = jnp.where(lane < hd // 2, product, 0.0)
    high = jnp.where(lane < hd // 2, 0.0, product)
    fresh = [
        jnp.sum(half, axis=1, keepdims=True) * ((hd // 2) ** (-0.5)) for half in (low, high)
    ]
    value_new = v_own[...].astype(F32)
    wait_recv(l_copies)
    stats = []
    for start in range(0, n_kv, 16):
        owners = range(start, min(start + 16, n_kv))
        stacked = pad_rows(jnp.concatenate([l_all[owner] for owner in owners], axis=0), 128)
        turned = jnp.transpose(stacked)
        stats += [turned[:rows, 8 * at : 8 * at + 2] for at in range(len(owners))]
    wait_recv(o_copies)
    maps = []
    for half in range(2):
        levels = [stat[:, half : half + 1] for stat in stats]
        peak = fresh[half]
        for level in levels:
            peak = jnp.maximum(peak, level)
        weight = jnp.exp(fresh[half] - peak)
        bottom = weight
        top = weight * value_new
        for owner in range(n_kv):
            weight = jnp.exp(levels[owner] - peak)
            bottom = bottom + weight
            top = top + weight * o_all[owner, half].astype(F32)
        maps.append(top / bottom)
    difference = maps[0] - lam[me // groups] * maps[1]
    normed = (
        difference
        * lax.rsqrt(jnp.mean(difference * difference, axis=1, keepdims=True) + epsilon)
        * head_gain[...]
    )
    h_all[me] = normed.astype(BF16)
    h_copies = exchange("kv", n_kv, lambda peer: h_all.at[me], h_all.at[me], h_s, h_r)
    loads[0].wait()
    wait_recv(h_copies)
    columns = []
    for head in range(n_kv // groups):
        if groups == 1:
            columns.append(h_all[head])
        else:
            columns.append(
                jnp.concatenate(
                    [h_all[head * groups + group].astype(F32) for group in range(groups)], axis=0
                )[:seqs].astype(BF16)
            )
    heads_out = jnp.concatenate(columns, axis=1)
    b_all[me_tp] = jnp.dot(heads_out, wo[...], preferred_element_type=F32).astype(BF16)
    b_copies = exchange("tp", n_tp, lambda peer: b_all.at[me_tp], b_all.at[me_tp], b_s, b_r)
    wait_recv(b_copies)
    branch = b_all[0].astype(F32)
    for index in range(1, n_tp):
        branch = branch + b_all[index].astype(F32)
    residual = (x[...].astype(F32) + branch).astype(BF16)
    res_f = residual.astype(F32)
    sq_all[me] = jnp.broadcast_to(jnp.sum(res_f * res_f, axis=1, keepdims=True), (seqs, 128))
    sq_copies = exchange("kv", n_kv, lambda peer: sq_all.at[me], sq_all.at[me], s_s, s_r)
    normed_mid = (res_f * mid_gain[...]).astype(BF16)
    for index, buf in enumerate((wg, wu)):
        loads[1 + index].wait()
        product = jnp.dot(normed_mid, buf[...], preferred_element_type=F32).astype(FF_LINK)
        product = pad_cols(product, n_kv * chunk)
        for owner in range(n_kv):
            gu_part[owner, index] = product[:, owner * chunk : (owner + 1) * chunk]
    gu_copies = exchange("kv", n_kv, lambda peer: gu_part.at[peer], gu_all.at[me], g_s, g_r)
    gu_all[me] = gu_part[me]
    wait_recv(sq_copies)
    square = sq_all[0]
    for index in range(1, n_kv):
        square = square + sq_all[index]
    scale = lax.rsqrt(square[:, :1] / width + epsilon)
    wait_recv(gu_copies)
    sums = []
    for index in range(2):
        total = gu_all[0, index].astype(F32)
        for owner in range(1, n_kv):
            total = total + gu_all[owner, index].astype(F32)
        sums.append(scale * total)
    hid_all[me] = (sums[0] / (1.0 + jnp.exp(-sums[0])) * sums[1]).astype(BF16)
    i_copies = exchange("kv", n_kv, lambda peer: hid_all.at[me], hid_all.at[me], i_s, i_r)
    loads[3].wait()
    wait_recv(i_copies)
    hidden = jnp.concatenate([hid_all[owner] for owner in range(n_kv)], axis=1)
    hidden = hidden[:, : wd.shape[0]]
    down = jnp.dot(hidden, wd[...], preferred_element_type=F32).astype(BF16)
    own = out.shape[1]
    for index in range(n_tp):
        d_part[index] = down[:, index * own : (index + 1) * own]
    d_copies = exchange("tp", n_tp, lambda peer: d_part.at[peer], d_all.at[me_tp], d_s, d_r)
    d_all[me_tp] = d_part[me_tp]
    base = res_f[:, :own]
    for index in range(1, n_tp):
        base = jnp.where(me_tp == index, res_f[:, index * own : (index + 1) * own], base)
    wait_recv(d_copies)
    mixer = d_all[0].astype(F32)
    for index in range(1, n_tp):
        mixer = mixer + d_all[index].astype(F32)
    out[...] = (base + mixer).astype(BF16)
    wait_send(
        l_copies + o_copies + h_copies + b_copies + sq_copies + gu_copies + i_copies + d_copies
    )


VM = pl.BlockSpec(memory_space=pltpu.VMEM)
ANY = pl.BlockSpec(memory_space=pl.ANY)


def per_device(
    n_kv, n_tp, tokens, attn_gain, w_query, w_key, w_value, cache_keys, cache_values, lambdas,
    head_gain, w_out, mlp_gain, w_gate, w_up, w_down,
):
    seqs, own = tokens.shape
    heads = lambdas.shape[0]
    hd = head_gain.shape[0]
    half = hd // 2
    feats = attn_gain.shape[0]
    width = feats * n_kv
    groups = n_kv // heads
    rows = -(-seqs // groups)
    positions = cache_keys.shape[1]
    units = w_gate.shape[1]
    chunk = 128 * -(-units // (128 * n_kv))
    dma = pltpu.SemaphoreType.DMA
    kv_sems = [dma((n_kv - 1,)), dma((n_kv - 1,))]
    tp_sems = [dma((n_tp - 1,)), dma((n_tp - 1,))]
    sds = jax.ShapeDtypeStruct

    x, q_all, k_own, v_own = pl.pallas_call(
        functools.partial(project_kernel, (n_kv, n_tp, groups, rows, width)),
        out_shape=[
            sds((seqs, feats), BF16), sds((n_kv, rows, hd), BF16),
            sds((rows, hd), BF16), sds((rows, hd), BF16),
        ],
        in_specs=[VM, VM, ANY, ANY, ANY],
        out_specs=[VM] * 4,
        scratch_shapes=[
            pltpu.VMEM((3, feats, heads * hd), BF16),
            pltpu.VMEM((n_tp, seqs, own), BF16),
            pltpu.VMEM((n_kv, seqs, 128), F32),
            pltpu.VMEM((n_kv, 3, rows, hd), QKV_LINK),
            pltpu.VMEM((n_kv, 3, rows, hd), QKV_LINK),
            dma((3,)), *tp_sems, *kv_sems, *kv_sems, *kv_sems,
        ],
        compiler_params=pltpu.CompilerParams(
            collective_id=0, has_side_effects=True, vmem_limit_bytes=24 << 20
        ),
        name="project",
    )(tokens, attn_gain.reshape(1, feats), w_query, w_key, w_value)

    q_heads = q_all.reshape(heads, groups * rows, hd)[:, :seqs]
    q_rows = jnp.transpose(q_heads, (1, 0, 2))
    zero = jnp.zeros_like(q_rows)
    first = lax.broadcasted_iota(jnp.int32, q_rows.shape, 2) < half
    q_blocks = jnp.concatenate(
        [jnp.where(first, q_rows, zero), jnp.where(first, zero, q_rows)], axis=1
    )
    per_step = 2 if seqs % 2 == 0 else 1
    length = positions * heads
    o_maps, l_maps = pl.pallas_call(
        functools.partial(attend_kernel, heads, per_step),
        out_shape=[sds((heads, 2, seqs, hd), BF16), sds((heads, 8, 128), F32)],
        grid=(seqs // per_step,),
        in_specs=[
            pl.BlockSpec((per_step, 2 * heads, hd), lambda i: (i, 0, 0)),
            pl.BlockSpec((per_step, length, hd), lambda i: (i, 0, 0)),
            pl.BlockSpec((per_step, length, hd), lambda i: (i, 0, 0)),
        ],
        out_specs=[
            pl.BlockSpec((heads, 2, seqs, hd), lambda i: (0, 0, 0, 0)),
            pl.BlockSpec((heads, 8, 128), lambda i: (0, 0, 0)),
        ],
        scratch_shapes=[
            pltpu.VMEM((2 * heads, seqs, hd), F32),
            pltpu.VMEM((2 * heads, 128), F32),
        ],
        compiler_params=pltpu.CompilerParams(vmem_limit_bytes=24 << 20),
        name="attend",
    )(
        q_blocks,
        cache_keys.reshape(seqs, length, hd),
        cache_values.reshape(seqs, length, hd),
    )
    if groups > 1:
        extra = groups * rows - seqs
        o_maps = jnp.pad(o_maps, ((0, 0), (0, 0), (0, extra), (0, 0)))
        o_maps = o_maps.reshape(heads, 2, groups, rows, hd).transpose(0, 2, 1, 3, 4)
        o_maps = o_maps.reshape(n_kv, 2, rows, hd)
        l_maps = l_maps[:, :, : groups * rows].reshape(heads, 8, groups, rows)
        l_maps = l_maps.transpose(0, 2, 1, 3).reshape(n_kv, 8, rows)
        l_maps = jnp.pad(l_maps, ((0, 0), (0, 0), (0, 128 - rows)))

    return pl.pallas_call(
        functools.partial(finish_kernel, (n_kv, n_tp, groups, rows, width, chunk)),
        out_shape=sds((seqs, own), BF16),
        in_specs=[pl.BlockSpec(memory_space=pltpu.SMEM)] + [VM] * 8 + [ANY] * 4,
        out_specs=VM,
        scratch_shapes=[
            pltpu.VMEM(w_out.shape, BF16),
            pltpu.VMEM(w_gate.shape, BF16),
            pltpu.VMEM(w_up.shape, BF16),
            pltpu.VMEM(w_down.shape, BF16),
            pltpu.VMEM((n_kv, 2, rows, hd), BF16),
            pltpu.VMEM((n_kv, 8, 128), F32),
            pltpu.VMEM((n_kv, rows, hd), BF16),
            pltpu.VMEM((n_tp, seqs, feats), BF16),
            pltpu.VMEM((n_kv, seqs, 128), F32),
            pltpu.VMEM((n_kv, 2, seqs, chunk), FF_LINK),
            pltpu.VMEM((n_kv, 2, seqs, chunk), FF_LINK),
            pltpu.VMEM((n_kv, seqs, chunk), BF16),
            pltpu.VMEM((n_tp, seqs, own), BF16),
            pltpu.VMEM((n_tp, seqs, own), BF16),
            dma((4,)), *kv_sems, *kv_sems, *kv_sems, *tp_sems,
            *kv_sems, *kv_sems, *kv_sems, *tp_sems,
        ],
        compiler_params=pltpu.CompilerParams(
            collective_id=1, has_side_effects=True, vmem_limit_bytes=30 << 20
        ),
        name="finish",
    )(
        lambdas, o_maps, l_maps, q_all, k_own, v_own, head_gain.reshape(1, hd), x,
        mlp_gain.reshape(1, feats), w_out, w_gate, w_up, w_down,
    )


def solution(mesh):
    in_specs = (
        P(None, ("kv", "tp")), P("kv"), P("kv", "tp"), P("kv", "tp"), P("kv", "tp"),
        P(None, "kv", "tp", None), P(None, "kv", "tp", None), P("tp"), P(),
        P("tp", "kv"), P("kv"), P("kv", "tp"), P("kv", "tp"), P("tp", "kv"),
    )
    return jax.shard_map(
        functools.partial(per_device, mesh.shape["kv"], mesh.shape["tp"]),
        mesh=mesh, in_specs=in_specs, out_specs=P(None, ("kv", "tp")), check_vma=False,
    )
```

```python
import functools

import jax
import jax.numpy as jnp
from jax import lax
from jax.experimental import pallas as pl
from jax.experimental.pallas import tpu as pltpu
from jax.sharding import PartitionSpec as P

epsilon = 1e-06
MESH = pl.DeviceIdType.MESH
F32 = jnp.float32
BF16 = jnp.bfloat16
Q_LINK = jnp.bfloat16
KV_LINK = jnp.float32
FF_LINK = jnp.bfloat16


def peers(axis, count):
    me = lax.axis_index(axis)
    return [(step, lax.rem(me + step, count)) for step in range(1, count)]


def greet(n_kv, n_tp):
    barrier = pltpu.get_barrier_semaphore()
    for axis, count in (("kv", n_kv), ("tp", n_tp)):
        for _, peer in peers(axis, count):
            pl.semaphore_signal(barrier, inc=1, device_id={axis: peer}, device_id_type=MESH)
    pl.semaphore_wait(barrier, n_kv + n_tp - 2)


def exchange(axis, count, source, target, send_sem, recv_sem):
    copies = []
    for step, peer in peers(axis, count):
        copy = pltpu.make_async_remote_copy(
            src_ref=source(peer),
            dst_ref=target,
            send_sem=send_sem.at[step - 1],
            recv_sem=recv_sem.at[step - 1],
            device_id={axis: peer},
            device_id_type=MESH,
        )
        copy.start()
        copies.append(copy)
    return copies


def wait_recv(copies):
    for copy in copies:
        copy.wait_recv()


def wait_send(copies):
    for copy in copies:
        copy.wait_send()


def pad_rows(value, rows):
    if value.shape[0] == rows:
        return value
    return jnp.concatenate(
        [value, jnp.zeros((rows - value.shape[0],) + value.shape[1:], value.dtype)], axis=0
    )


def pad_cols(value, cols):
    if value.shape[1] == cols:
        return value
    return jnp.concatenate(
        [value, jnp.zeros((value.shape[0], cols - value.shape[1]), value.dtype)], axis=1
    )


def layer_kernel(
    dims, tok_in, gain_in, wq_in, wk_in, wv_in, keys_in, values_in, lam_in, head_gain_in, w_out_in,
    mid_gain_in, w_gate_in, w_up_in, w_down_in,
    out,
    tok, gain, lam, head_gain, mid_gain, wq, wk, wv, keys, values, wo, wg, wu, wd,
    tok_all, sq_all, q_part, q_got, kv_part, kv_got, q_all, q_seq, acc, lse,
    o_in, o_all, l_in, l_all, h_all, b_all, mid_all, gu_part, gu_all, hid_all, d_part, d_all,
    w_sem, k_sem, v_sem, *sems,
):
    n_kv, n_tp, groups, rows, width, chunk, per_step = dims
    seqs, own = out.shape
    heads = n_kv // groups
    hd = head_gain.shape[1]
    half_dim = hd // 2
    score_scale = half_dim ** (-0.5)
    length = keys.shape[1]
    steps = seqs // per_step
    pairs = [(sems[2 * at], sems[2 * at + 1]) for at in range(len(sems) // 2)]
    t_sem, sq_sem, q_sem, qa_sem, kv_sem, l_sem, o_sem, h_sem, b_sem, m_sem = pairs[:10]
    g_sems, i_sem, d_sem = pairs[10:12], pairs[12], pairs[13]

    def load(index, source, target):
        copy = pltpu.make_async_copy(source, target, w_sem.at[index])
        copy.start()
        return copy

    load_tok = load(0, tok_in, tok)
    load_gain = load(1, gain_in, gain)
    load_q = load(2, wq_in, wq)
    load_k = load(3, wk_in, wk)
    load_v = load(4, wv_in, wv)

    def cache_copies(step):
        at = pl.ds(step * per_step, per_step)
        return (
            pltpu.make_async_copy(keys_in.at[at], keys.at[at], k_sem.at[step]),
            pltpu.make_async_copy(values_in.at[at], values.at[at], v_sem.at[step]),
        )

    for step in range(steps):
        for copy in cache_copies(step):
            copy.start()
    load_lam = load(5, lam_in, lam)
    load_hg = load(6, head_gain_in, head_gain)
    load_mg = load(7, mid_gain_in, mid_gain)
    load_wo = load(8, w_out_in, wo)
    load_wg = load(9, w_gate_in, wg)
    load_wu = load(10, w_up_in, wu)
    units = w_down_in.shape[0]
    load_wd = load(11, w_down_in, wd.at[pl.ds(0, units)])
    if units < n_kv * chunk:
        wd[units:, :] = jnp.zeros((n_kv * chunk - units, wd.shape[1]), BF16)

    greet(n_kv, n_tp)
    me = lax.axis_index("kv")
    me_tp = lax.axis_index("tp")
    load_tok.wait()
    tok_copies = exchange("tp", n_tp, lambda peer: tok, tok_all.at[me_tp], *t_sem)
    tok_all[me_tp] = tok[...]
    load_gain.wait()
    wait_recv(tok_copies)
    xf = jnp.concatenate([tok_all[index] for index in range(n_tp)], axis=1).astype(F32)
    normed = (xf * gain[...]).astype(BF16)

    def project(buf, part, index, link):
        product = jnp.dot(normed, buf[...], preferred_element_type=F32).astype(link)
        product = pad_rows(product, groups * rows)
        for owner in range(n_kv):
            head, group = owner // groups, owner % groups
            part[owner, index] = product[
                group * rows : (group + 1) * rows, head * hd : (head + 1) * hd
            ]

    def gathered_sum(got, index):
        total = got[0, index].astype(F32)
        for owner in range(1, n_kv):
            total = total + got[owner, index].astype(F32)
        return total

    load_q.wait()
    project(wq, q_part, 0, Q_LINK)
    q_copies = exchange("kv", n_kv, lambda peer: q_part.at[peer], q_got.at[me], *q_sem)
    q_got[me] = q_part[me]
    sq_all[me] = jnp.broadcast_to(jnp.sum(xf * xf, axis=1, keepdims=True), (seqs, 128))
    sq_copies = exchange("kv", n_kv, lambda peer: sq_all.at[me], sq_all.at[me], *sq_sem)
    load_k.wait()
    project(wk, kv_part, 0, KV_LINK)
    load_v.wait()
    project(wv, kv_part, 1, KV_LINK)
    kv_got[me] = kv_part[me]
    wait_recv(q_copies)
    total = gathered_sum(q_got, 0)
    wait_recv(sq_copies)
    square = sq_all[0]
    for index in range(1, n_kv):
        square = square + sq_all[index]
    scale = lax.rsqrt(square[:, :1] / width + epsilon)
    if groups > 1:
        scale = pad_rows(scale, groups * rows)
        group_of = lax.rem(me, groups)
        mine = scale[:rows]
        for group in range(1, groups):
            mine = jnp.where(group_of == group, scale[group * rows : (group + 1) * rows], mine)
        scale = mine
    q_own = (scale * total).astype(BF16)
    q_all[me] = q_own
    qa_copies = exchange("kv", n_kv, lambda peer: q_all.at[me], q_all.at[me], *qa_sem)
    kv_copies = exchange("kv", n_kv, lambda peer: kv_part.at[peer], kv_got.at[me], *kv_sem)
    wait_recv(qa_copies)
    for owner in range(n_kv):
        head, group = owner // groups, owner % groups
        q_seq[group * rows : (group + 1) * rows, head : head + 1, :] = q_all[owner].astype(F32)[
            :, None, :
        ]

    row = lax.broadcasted_iota(jnp.int32, (2 * heads * per_step, length), 0)
    col = lax.broadcasted_iota(jnp.int32, (2 * heads * per_step, length), 1)
    keep = lax.rem(col, heads) == lax.rem(row, heads)
    stat_lane = lax.broadcasted_iota(jnp.int32, (2 * heads, 128), 1)
    q_lane = lax.broadcasted_iota(jnp.int32, (heads, hd), 1)
    lse[...] = jnp.zeros_like(lse)
    l_in[...] = jnp.zeros_like(l_in)

    def queries(seq):
        vec = q_seq[seq]
        return jnp.concatenate(
            [jnp.where(q_lane < half_dim, vec, 0.0), jnp.where(q_lane < half_dim, 0.0, vec)],
            axis=0,
        ).astype(BF16)

    def wide(parts):
        return parts[0] if per_step == 1 else jnp.concatenate(parts, axis=1)

    def attend(at):
        span = range(at * per_step, (at + 1) * per_step)
        blank = jnp.zeros((2 * heads, hd), BF16)
        query = jnp.concatenate(
            [wide([queries(seq) if other == seq else blank for other in span]) for seq in span],
            axis=0,
        )
        scores = lax.dot_general(
            query, wide([keys[seq] for seq in span]), (((1,), (1,)), ((), ())),
            preferred_element_type=F32,
        )
        scores = jnp.where(keep, scores * score_scale, -jnp.inf)
        peak = jnp.max(scores, axis=1, keepdims=True)
        weights = jnp.exp(scores - peak)
        total = jnp.sum(weights, axis=1, keepdims=True)
        summed = jnp.dot(
            weights.astype(BF16), wide([values[seq] for seq in span]), preferred_element_type=F32
        )
        result = summed / total
        level = peak + jnp.log(total)
        stats = lse[...]
        for index, seq in enumerate(span):
            part = slice(index * 2 * heads, (index + 1) * 2 * heads)
            acc[:, seq : seq + 1, :] = result[part, index * hd : (index + 1) * hd][:, None, :]
            stats = jnp.where(stat_lane == seq, level[part], stats)
        lse[...] = stats

    for step in range(steps):
        for copy in cache_copies(step):
            copy.wait()
    for step in range(steps):
        attend(step)

    for owner in range(n_kv):
        head, group = owner // groups, owner % groups
        span = slice(group * rows, (group + 1) * rows)
        for half in range(2):
            at = half * heads + head
            l_in[owner, half : half + 1, :] = pad_cols(lse[at : at + 1, span], 128)
    l_copies = exchange("kv", n_kv, lambda peer: l_in.at[peer], l_all.at[me], *l_sem)
    for owner in range(n_kv):
        head, group = owner // groups, owner % groups
        span = slice(group * rows, (group + 1) * rows)
        for half in range(2):
            o_in[owner, half] = acc[half * heads + head, span, :].astype(BF16)
    o_copies = exchange("kv", n_kv, lambda peer: o_in.at[peer], o_all.at[me], *o_sem)
    l_all[me] = l_in[me]
    o_all[me] = o_in[me]
    wait_recv(kv_copies)
    k_own = (scale * gathered_sum(kv_got, 0)).astype(BF16).astype(F32)
    value_new = (scale * gathered_sum(kv_got, 1)).astype(BF16).astype(F32)
    product = q_own.astype(F32) * k_own
    lane = lax.broadcasted_iota(jnp.int32, product.shape, 1)
    low = jnp.where(lane < half_dim, product, 0.0)
    high = jnp.where(lane < half_dim, 0.0, product)
    fresh = [jnp.sum(part, axis=1, keepdims=True) * score_scale for part in (low, high)]
    load_lam.wait()
    load_hg.wait()
    load_mg.wait()
    at_head = lax.broadcasted_iota(jnp.int32, lam.shape, 1) == me // groups
    lam_own = jnp.sum(jnp.where(at_head, lam[...], 0.0), axis=1, keepdims=True)
    wait_recv(l_copies)
    stats = []
    for start in range(0, n_kv, 16):
        owners = range(start, min(start + 16, n_kv))
        stacked = pad_rows(jnp.concatenate([l_all[owner] for owner in owners], axis=0), 128)
        turned = jnp.transpose(stacked)
        stats += [turned[:rows, 8 * at : 8 * at + 2] for at in range(len(owners))]
    wait_recv(o_copies)
    maps = []
    for half in range(2):
        levels = [stat[:, half : half + 1] for stat in stats]
        peak = fresh[half]
        for level in levels:
            peak = jnp.maximum(peak, level)
        weight = jnp.exp(fresh[half] - peak)
        bottom = weight
        top = weight * value_new
        for owner in range(n_kv):
            weight = jnp.exp(levels[owner] - peak)
            bottom = bottom + weight
            top = top + weight * o_all[owner, half].astype(F32)
        maps.append(top / bottom)
    difference = maps[0] - lam_own * maps[1]
    normed = (
        difference
        * lax.rsqrt(jnp.mean(difference * difference, axis=1, keepdims=True) + epsilon)
        * head_gain[...]
    )
    h_all[me] = normed.astype(BF16)
    h_copies = exchange("kv", n_kv, lambda peer: h_all.at[me], h_all.at[me], *h_sem)
    load_wo.wait()
    wait_recv(h_copies)
    columns = []
    for head in range(n_kv // groups):
        if groups == 1:
            columns.append(h_all[head])
        else:
            columns.append(
                jnp.concatenate(
                    [h_all[head * groups + group].astype(F32) for group in range(groups)], axis=0
                )[:seqs].astype(BF16)
            )
    heads_out = jnp.concatenate(columns, axis=1)
    b_all[me_tp] = jnp.dot(heads_out, wo[...], preferred_element_type=F32).astype(BF16)
    b_copies = exchange("tp", n_tp, lambda peer: b_all.at[me_tp], b_all.at[me_tp], *b_sem)
    wait_recv(b_copies)
    branch = b_all[0].astype(F32)
    for index in range(1, n_tp):
        branch = branch + b_all[index].astype(F32)
    residual = (xf + branch).astype(BF16)
    res_f = residual.astype(F32)
    mid_all[me] = jnp.broadcast_to(jnp.sum(res_f * res_f, axis=1, keepdims=True), (seqs, 128))
    mid_copies = exchange("kv", n_kv, lambda peer: mid_all.at[me], mid_all.at[me], *m_sem)
    normed_mid = (res_f * mid_gain[...]).astype(BF16)
    gu_copies = []
    for index, (ready, buf) in enumerate(((load_wg, wg), (load_wu, wu))):
        ready.wait()
        product = lax.dot_general(
            normed_mid, buf[...], (((1,), (1,)), ((), ())), preferred_element_type=F32
        ).astype(FF_LINK)
        product = pad_cols(product, n_kv * chunk)
        for owner in range(n_kv):
            gu_part[index, owner] = product[:, owner * chunk : (owner + 1) * chunk]
        gu_copies += exchange(
            "kv", n_kv, lambda peer: gu_part.at[index, peer], gu_all.at[index, me], *g_sems[index]
        )
        gu_all[index, me] = gu_part[index, me]
    wait_recv(mid_copies)
    square = mid_all[0]
    for index in range(1, n_kv):
        square = square + mid_all[index]
    scale = lax.rsqrt(square[:, :1] / width + epsilon)
    wait_recv(gu_copies)
    sums = []
    for index in range(2):
        total = gu_all[index, 0].astype(F32)
        for owner in range(1, n_kv):
            total = total + gu_all[index, owner].astype(F32)
        sums.append(scale * total)
    hid_all[me] = (sums[0] / (1.0 + jnp.exp(-sums[0])) * sums[1]).astype(BF16)
    i_copies = exchange("kv", n_kv, lambda peer: hid_all.at[me], hid_all.at[me], *i_sem)
    load_wd.wait()
    down = None
    for step in range(n_kv):
        if step > 0:
            i_copies[step - 1].wait_recv()
        owner = lax.rem(me + n_kv - step, n_kv)
        share = jnp.dot(
            hid_all[owner],
            wd[pl.ds(pl.multiple_of(owner * chunk, chunk), chunk), :],
            preferred_element_type=F32,
        )
        down = share if down is None else down + share
    down = down.astype(BF16)
    own = out.shape[1]
    for index in range(n_tp):
        d_part[index] = down[:, index * own : (index + 1) * own]
    d_copies = exchange("tp", n_tp, lambda peer: d_part.at[peer], d_all.at[me_tp], *d_sem)
    d_all[me_tp] = d_part[me_tp]
    base = res_f[:, :own]
    for index in range(1, n_tp):
        base = jnp.where(me_tp == index, res_f[:, index * own : (index + 1) * own], base)
    wait_recv(d_copies)
    mixer = d_all[0].astype(F32)
    for index in range(1, n_tp):
        mixer = mixer + d_all[index].astype(F32)
    out[...] = (base + mixer).astype(BF16)
    wait_send(
        tok_copies + q_copies + sq_copies + qa_copies + kv_copies + l_copies + o_copies
        + h_copies + b_copies + mid_copies + gu_copies + i_copies + d_copies
    )


ANY = pl.BlockSpec(memory_space=pl.ANY)


def per_device(
    n_kv, n_tp, tokens, attn_gain, w_query, w_key, w_value, cache_keys, cache_values, lambdas,
    head_gain, w_out, mlp_gain, w_gate, w_up, w_down,
):
    seqs, own = tokens.shape
    heads = lambdas.shape[0]
    hd = head_gain.shape[0]
    feats = attn_gain.shape[0]
    width = feats * n_kv
    groups = n_kv // heads
    rows = -(-seqs // groups)
    units = w_gate.shape[1]
    chunk = 128 * -(-units // (128 * n_kv))
    length = cache_keys.shape[1] * heads
    per_step = 2 if seqs % 2 == 0 else 1
    dma = pltpu.SemaphoreType.DMA
    kv_sems = [dma((n_kv - 1,)), dma((n_kv - 1,))]
    tp_sems = [dma((n_tp - 1,)), dma((n_tp - 1,))]
    vm = pltpu.VMEM
    return pl.pallas_call(
        functools.partial(layer_kernel, (n_kv, n_tp, groups, rows, width, chunk, per_step)),
        out_shape=jax.ShapeDtypeStruct((seqs, own), BF16),
        in_specs=[ANY] * 14,
        out_specs=pl.BlockSpec(memory_space=pltpu.VMEM),
        scratch_shapes=[
            vm((seqs, own), BF16),
            vm((1, feats), F32),
            vm((1, heads), F32),
            vm((1, hd), F32),
            vm((1, feats), F32),
            vm(w_query.shape, BF16),
            vm(w_key.shape, BF16),
            vm(w_value.shape, BF16),
            vm((seqs, length, hd), BF16),
            vm((seqs, length, hd), BF16),
            vm(w_out.shape, BF16),
            vm((units, feats), BF16),
            vm((units, feats), BF16),
            vm((n_kv * chunk, w_down.shape[1]), BF16),
            vm((n_tp, seqs, own), BF16),
            vm((n_kv, seqs, 128), F32),
            vm((n_kv, 1, rows, hd), Q_LINK),
            vm((n_kv, 1, rows, hd), Q_LINK),
            vm((n_kv, 2, rows, hd), KV_LINK),
            vm((n_kv, 2, rows, hd), KV_LINK),
            vm((n_kv, rows, hd), BF16),
            vm((groups * rows, heads, hd), F32),
            vm((2 * heads, groups * rows, hd), F32),
            vm((2 * heads, 128), F32),
            vm((n_kv, 2, rows, hd), BF16),
            vm((n_kv, 2, rows, hd), BF16),
            vm((n_kv, 8, 128), F32),
            vm((n_kv, 8, 128), F32),
            vm((n_kv, rows, hd), BF16),
            vm((n_tp, seqs, feats), BF16),
            vm((n_kv, seqs, 128), F32),
            vm((2, n_kv, seqs, chunk), FF_LINK),
            vm((2, n_kv, seqs, chunk), FF_LINK),
            vm((n_kv, seqs, chunk), BF16),
            vm((n_tp, seqs, own), BF16),
            vm((n_tp, seqs, own), BF16),
            dma((12,)), dma((seqs // per_step,)), dma((seqs // per_step,)),
            *tp_sems, *(kv_sems * 7), *tp_sems, *(kv_sems * 4), *tp_sems,
        ],
        compiler_params=pltpu.CompilerParams(
            collective_id=0, has_side_effects=True, vmem_limit_bytes=62 << 20
        ),
        name="layer",
    )(
        tokens, attn_gain.reshape(1, feats), w_query, w_key, w_value,
        cache_keys.reshape(seqs, length, hd), cache_values.reshape(seqs, length, hd),
        lambdas.reshape(1, heads), head_gain.reshape(1, hd), w_out, mlp_gain.reshape(1, feats),
        w_gate.T, w_up.T, w_down,
    )


def solution(mesh):
    in_specs = (
        P(None, ("kv", "tp")), P("kv"), P("kv", "tp"), P("kv", "tp"), P("kv", "tp"),
        P(None, "kv", "tp", None), P(None, "kv", "tp", None), P("tp"), P(),
        P("tp", "kv"), P("kv"), P("kv", "tp"), P("kv", "tp"), P("tp", "kv"),
    )
    return jax.shard_map(
        functools.partial(per_device, mesh.shape["kv"], mesh.shape["tp"]),
        mesh=mesh, in_specs=in_specs, out_specs=P(None, ("kv", "tp")), check_vma=False,
    )
```
